32 devices in a mesh: ep: 4 (over y, x), tp: 8 (over z, core).
Axes of the slice: x: 2, y: 2, z: 4, core: 2. Of those that a mesh axis runs over, the one named last changes fastest.
Arguments:
- tokens: bfloat16 [64, 4096], P(None, 'ep'), may hold values from -60 to 60
- gain_attn: bfloat16 [4096], P('ep'), may hold values from 0.099609375 to 1.8984375
- w_query: bfloat16 [4096, 2048], P('ep', 'tp'), may hold values from -0.09375 to 0.09375
- w_key: bfloat16 [4096, 2048], P('ep', 'tp'), may hold values from -0.09375 to 0.09375
- w_value: bfloat16 [4096, 2048], P('ep', 'tp'), may hold values from -0.09375 to 0.09375
- w_output: bfloat16 [2048, 4096], P('tp', 'ep'), may hold values from -0.125 to 0.125
- key_cache: bfloat16 [64, 1024, 2048], P('ep', None, 'tp'), may hold values from -6 to 6
- value_cache: bfloat16 [64, 1024, 2048], P('ep', None, 'tp'), may hold values from -10 to 10
- lengths: int32 [64], P('ep'), may hold values from 128 to 1024
- score_shift: float32 [16], P('tp'), may hold values from -9.5 to -3.5
- gain_ffn: bfloat16 [4096], replicated, may hold values from 0.099609375 to 1.8984375
- w_mix: bfloat16 [4096], P('ep'), may hold values from -0.09375 to 0.09375
- w_dense_gate: bfloat16 [4096, 4096], P('ep', 'tp'), may hold values from -0.09375 to 0.09375
- w_dense_up: bfloat16 [4096, 4096], P('ep', 'tp'), may hold values from -0.09375 to 0.09375
- w_dense_down: bfloat16 [4096, 4096], P('tp', 'ep'), may hold values from -0.09375 to 0.09375
- route_group: int32 [64], replicated, may hold values from 0 to 3, as said below
- route_inner: int32 [64, 2], replicated, may hold values from 0 to 3, as said below
- route_weight: float32 [64, 2], replicated, may hold values from 0.3 to 1
- w_exp_gate: bfloat16 [16, 4096, 2048], P('ep', None, 'tp'), may hold values from -0.09375 to 0.09375
- w_exp_up: bfloat16 [16, 4096, 2048], P('ep', None, 'tp'), may hold values from -0.09375 to 0.09375
- w_exp_down: bfloat16 [16, 2048, 4096], P('ep', 'tp'), may hold values from -0.125 to 0.125
Outputs:
- mixed: bfloat16 [64, 4096], P(None, 'ep')
- new_keys: bfloat16 [64, 2048], P('ep', 'tp')
- new_values: bfloat16 [64, 2048], P('ep', 'tp')
The draws below stay inside these ranges and needn't reach their ends.
Inputs may be any that keep to these rules, and one draw needn't show every extreme that they name: `route_group`: within every aligned block of 16 sequences (the sequences of one index of ep) exactly half of the tokens use one group, the same group in every block; the other groups share the rest. A token's 2 experts inside its group differ. Within every aligned block of 16 sequences no expert (route_group * 4 + route_inner) is used by more than 4 tokens, and the experts of the group that half of the block uses are each used by exactly 4.
All inputs are finite; a program needn't handle non-finite values.
Results may differ from the reference program's by a relative error of at most 0.0039.
The reference program's roundings to bfloat16 on the way count: a program that leaves them out, or rounds other values in their place, can miss the bound.
Values may be sent and summed in bfloat16 or wider, within the bound.
A program may use at most 128 MiB of HBM per device.

```python
import math
import jax
import jax.numpy as jnp
from jax import lax

D = 4096
HEADS = 16
HD = 128
FF = 2048
FFD = 4096
GROUPS = 4
EPG = 4
TOPK = 2
SEQ_DEV = 16
CACHE_LEN = 1024
BATCH = 64
EXPERTS = 16
ATT = 2048
N_EP = 4


def draw_tokens(key, part):
    column_block = jnp.arange(D) // (D // N_EP)
    rising = jnp.exp(jnp.log(3.0) * column_block / max(N_EP - 1, 1))
    base_part = jnp.clip(jax.random.normal(key, (BATCH, D), jnp.float32), -6.0, 6.0)
    return (base_part * rising[None, :]).astype(jnp.bfloat16)


def draw_value_cache(key, part):
    common = jnp.clip(jax.random.normal(jax.random.fold_in(key, 3), (BATCH, 1, ATT), jnp.float32), -5.0, 5.0)
    fresh_part = jnp.clip(jax.random.normal(jax.random.fold_in(key, 4), (BATCH, CACHE_LEN, ATT), jnp.float32), -5.0, 5.0)
    return (0.8 * common + 0.6 * fresh_part).astype(jnp.bfloat16)


def draw_score_shift(key, part):
    return jax.random.uniform(key, (HEADS,), jnp.float32, -9.0, -3.5)


def shuffle_many(subkeys, length):

    def shuffle_one(subkey):
        return jax.random.permutation(subkey, length)
    return jax.vmap(shuffle_one)(subkeys)


def route_table(key):
    base_key = jax.random.fold_in(key, 17)
    blocks = BATCH // SEQ_DEV
    half_block = SEQ_DEV // 2
    favored = jax.random.randint(jax.random.fold_in(base_key, 1), (), 0, GROUPS)
    first_share = jax.random.randint(jax.random.fold_in(base_key, 2), (blocks,), 0, half_block + 1)
    second_share = jax.random.randint(jax.random.fold_in(base_key, 3), (blocks,), 0, half_block + 1 - first_share)
    rotation = jax.random.randint(jax.random.fold_in(base_key, 4), (blocks,), 0, 3)
    position = jnp.arange(SEQ_DEV)[None, :]
    remaining = position - half_block
    other_slot = jnp.where(remaining < first_share[:, None], 0, jnp.where(remaining < first_share[:, None] + second_share[:, None], 1, 2))
    group_label = jnp.where(position < half_block, favored, (favored + 1 + (other_slot + rotation[:, None]) % 3) % GROUPS)
    shuffle_order = shuffle_many(jax.random.split(jax.random.fold_in(base_key, 5), blocks), SEQ_DEV)
    group_of = jnp.take_along_axis(group_label, shuffle_order, axis=1)
    same_group = (group_of[:, :, None] == jnp.arange(GROUPS)[None, None, :]).astype(jnp.int32)
    before = jnp.cumsum(same_group, axis=1) - same_group
    slot_rank = jnp.sum(before * same_group, axis=2)
    cycles = shuffle_many(jax.random.split(jax.random.fold_in(base_key, 6), blocks * GROUPS), EPG).reshape(blocks, GROUPS, EPG)
    cycle_of = jnp.sum(same_group[:, :, :, None] * cycles[:, None, :, :], axis=2)
    inner_range = jnp.arange(EPG)[None, None, :]
    first_pick = jnp.sum(cycle_of * (inner_range == (slot_rank % EPG)[:, :, None]), axis=2)
    second_pick = jnp.sum(cycle_of * (inner_range == ((slot_rank + 1) % EPG)[:, :, None]), axis=2)
    inner_pick = jnp.stack([first_pick, second_pick], axis=2).reshape(BATCH, 2)
    return (group_of.reshape(BATCH).astype(jnp.int32), inner_pick.astype(jnp.int32))


def draw_route_group(key, part):
    return route_table(key)[0]


def draw_route_inner(key, part):
    return route_table(key)[1]


def set_ends(array, stream_key, smallest, high):
    spot = [jax.random.randint(jax.random.fold_in(stream_key, axis), (), 0, length) for axis, length in enumerate(array.shape)]
    main_axis = array.shape.index(max(array.shape))
    next_to = spot[:main_axis] + [(spot[main_axis] + 1) % array.shape[main_axis]] + spot[main_axis + 1:]
    return array.at[tuple(spot)].set(smallest).at[tuple(next_to)].set(high)


def steps_of(stream_key, dims, cuts, low, top_value):
    def one(axis_at, shards_of):
        draws = jax.random.uniform(jax.random.fold_in(jax.random.fold_in(stream_key, 6), axis_at), (shards_of,), jnp.float32, low / len(cuts), top_value / len(cuts))
        return jnp.repeat(jnp.exp(draws), dims[axis_at] // shards_of).reshape((-1,) + (1,) * (len(dims) - axis_at - 1))

    gain = one(*cuts[0])
    for cut in cuts[1:]:
        gain = gain * one(*cut)
    return gain


def normal_values(key, dims, width, reach, cuts=(), kind=jnp.bfloat16):
    drawn = width * jax.random.normal(key, dims, jnp.float32)
    if cuts:
        drawn = drawn * steps_of(key, dims, cuts, -0.22, 0.18)
    return jnp.clip(drawn, -reach, reach).astype(kind)


def setup_inputs(seed: int = 0) -> dict:
    keys = jax.random.split(jax.random.key(seed), 22)
    tokens = draw_tokens(jax.random.fold_in(keys[21], 71), 0)
    gain_attn = jnp.clip(1.0 + 0.18 * jax.random.normal(keys[1], (D,), jnp.float32), 0.099609375, 1.8984375).astype(jnp.bfloat16)
    w_query = normal_values(keys[2], (D, ATT), D ** -0.5, 0.09375, ((0, 4), (1, 8)))
    w_key = normal_values(keys[3], (D, ATT), D ** -0.5, 0.09375, ((0, 4), (1, 8)))
    w_value = normal_values(keys[4], (D, ATT), D ** -0.5, 0.09375, ((0, 4), (1, 8)))
    w_output = normal_values(keys[5], (ATT, D), ATT ** -0.5, 0.125, ((0, 8), (1, 4)))
    key_cache = normal_values(keys[6], (BATCH, CACHE_LEN, ATT), 1.0, 6.0, ((0, 4), (2, 8)))
    value_cache = draw_value_cache(jax.random.fold_in(keys[21], 71), 0)
    lengths = set_ends(jax.random.randint(keys[8], (BATCH,), CACHE_LEN // 8, CACHE_LEN + 1), jax.random.fold_in(keys[8], 1), CACHE_LEN // 8, CACHE_LEN).astype(jnp.int32)
    score_shift = draw_score_shift(jax.random.fold_in(keys[21], 71), 0)
    gain_ffn = jnp.clip(1.0 + 0.18 * jax.random.normal(keys[10], (D,), jnp.float32), 0.099609375, 1.8984375).astype(jnp.bfloat16)
    w_mix = normal_values(keys[11], (D,), D ** -0.5, 0.09375, ((0, 4),))
    w_dense_gate = normal_values(keys[12], (D, FFD), D ** -0.5, 0.09375, ((0, 4), (1, 8)))
    w_dense_up = normal_values(keys[13], (D, FFD), D ** -0.5, 0.09375, ((0, 4), (1, 8)))
    w_dense_down = normal_values(keys[14], (FFD, D), FFD ** -0.5, 0.09375, ((0, 8), (1, 4)))
    route_group = draw_route_group(jax.random.fold_in(keys[21], 71), 0)
    route_inner = draw_route_inner(jax.random.fold_in(keys[21], 71), 0)
    route_weight = jnp.clip(jax.random.uniform(keys[17], (BATCH, TOPK), jnp.float32, 0.3, 1.0), 0.3, 1.0)
    w_exp_gate = normal_values(keys[18], (EXPERTS, D, FF), D ** -0.5, 0.09375, ((0, 4), (2, 8)))
    w_exp_up = normal_values(keys[19], (EXPERTS, D, FF), D ** -0.5, 0.09375, ((0, 4), (2, 8)))
    w_exp_down = normal_values(keys[20], (EXPERTS, FF, D), FF ** -0.5, 0.125, ((0, 4), (1, 8)))
    return {"tokens": tokens, "gain_attn": gain_attn, "w_query": w_query, "w_key": w_key, "w_value": w_value, "w_output": w_output, "key_cache": key_cache, "value_cache": value_cache, "lengths": lengths, "score_shift": score_shift, "gain_ffn": gain_ffn, "w_mix": w_mix, "w_dense_gate": w_dense_gate, "w_dense_up": w_dense_up, "w_dense_down": w_dense_down, "route_group": route_group, "route_inner": route_inner, "route_weight": route_weight, "w_exp_gate": w_exp_gate, "w_exp_up": w_exp_up, "w_exp_down": w_exp_down}


norm_eps = 1e-06

def reference(tokens, gain_attn, w_query, w_key, w_value, w_output, key_cache, value_cache, lengths, score_shift, gain_ffn, w_mix, w_dense_gate, w_dense_up, w_dense_down, route_group, route_inner, route_weight, w_exp_gate, w_exp_up, w_exp_down):
    tokens_float = tokens.astype(jnp.float32)
    inv_first = lax.rsqrt(lax.optimization_barrier(jnp.mean(tokens_float * tokens_float, axis=1, keepdims=True)) + norm_eps)
    scaled_in = (tokens_float * gain_attn.astype(jnp.float32)).astype(jnp.bfloat16)
    queries = (jnp.dot(scaled_in, w_query, preferred_element_type=jnp.float32) * inv_first).astype(jnp.bfloat16)
    new_keys = (jnp.dot(scaled_in, w_key, preferred_element_type=jnp.float32) * inv_first).astype(jnp.bfloat16)
    new_values = (jnp.dot(scaled_in, w_value, preferred_element_type=jnp.float32) * inv_first).astype(jnp.bfloat16)

    def attend_block(inputs):
        block_query, block_keys, block_values, block_lengths = inputs
        seq_count = block_query.shape[0]
        head_query = block_query.astype(jnp.float32).reshape(seq_count, HEADS, HD)
        head_keys = block_keys.astype(jnp.float32).reshape(seq_count, CACHE_LEN, HEADS, HD)
        scores = jnp.einsum('bhd,blhd->bhl', head_query, head_keys) / math.sqrt(HD) + score_shift[None, :, None]
        position = jnp.arange(CACHE_LEN, dtype=jnp.int32)
        live_mask = position[None, None, :] < block_lengths[:, None, None]
        soft_terms = jnp.where(live_mask, jax.nn.softplus(scores), 0.0)
        later_sum = lax.cumsum(soft_terms, axis=2, reverse=True) - soft_terms
        stick = jnp.where(live_mask, jnp.exp(jax.nn.log_sigmoid(scores) - later_sum), 0.0)
        stick = lax.optimization_barrier(stick.astype(jnp.bfloat16)).astype(jnp.float32)
        head_values = block_values.astype(jnp.float32).reshape(seq_count, CACHE_LEN, HEADS, HD)
        attended = jnp.einsum('bhl,blhd->bhd', stick, head_values)
        return attended.reshape(seq_count, ATT).astype(jnp.bfloat16)
    block_count = BATCH // SEQ_DEV
    attended = lax.map(attend_block, (queries.reshape(block_count, SEQ_DEV, ATT), key_cache.reshape(block_count, SEQ_DEV, CACHE_LEN, ATT), value_cache.reshape(block_count, SEQ_DEV, CACHE_LEN, ATT), lengths.reshape(block_count, SEQ_DEV))).reshape(BATCH, ATT)
    attn_out = jnp.dot(attended, w_output, preferred_element_type=jnp.float32)
    middle = (tokens_float + attn_out).astype(jnp.bfloat16)
    middle_float = middle.astype(jnp.float32)
    inv_second = lax.rsqrt(lax.optimization_barrier(jnp.mean(middle_float * middle_float, axis=1, keepdims=True)) + norm_eps)
    scaled_mid = (middle_float * gain_ffn.astype(jnp.float32)).astype(jnp.bfloat16)
    dense_pre = jnp.dot(scaled_mid, w_dense_gate, preferred_element_type=jnp.float32) * inv_second
    dense_lin = jnp.dot(scaled_mid, w_dense_up, preferred_element_type=jnp.float32) * inv_second
    dense_hidden = (jax.nn.silu(dense_pre) * dense_lin).astype(jnp.bfloat16)
    mix_gate = jax.nn.sigmoid(jnp.dot(scaled_mid, w_mix, preferred_element_type=jnp.float32) * inv_second[:, 0])
    dense_out = jnp.dot(dense_hidden, w_dense_down, preferred_element_type=jnp.float32) * mix_gate[:, None]
    expert_ids = (route_group[:, None] * EPG + route_inner).astype(jnp.int32)
    expert_range = jnp.arange(EXPERTS, dtype=jnp.int32)
    combine = lax.optimization_barrier(jnp.sum(jnp.where(expert_ids[:, :, None] == expert_range[None, None, :], route_weight[:, :, None], 0.0), axis=1))

    def add_expert(running, expert_index):
        gate_pre = jnp.dot(scaled_mid, w_exp_gate[expert_index], preferred_element_type=jnp.float32) * inv_second
        up_proj = jnp.dot(scaled_mid, w_exp_up[expert_index], preferred_element_type=jnp.float32) * inv_second
        hidden = (jax.nn.silu(gate_pre) * up_proj).astype(jnp.bfloat16)
        output_rows = jnp.dot(hidden, w_exp_down[expert_index], preferred_element_type=jnp.float32)
        weight_col = lax.dynamic_index_in_dim(combine, expert_index, 1, keepdims=True)
        return (running + output_rows * weight_col, None)
    expert_total, _ = lax.scan(add_expert, jnp.zeros((BATCH, D), jnp.float32), expert_range)
    mixed = (middle_float + expert_total + dense_out).astype(jnp.bfloat16)
    return (mixed, new_keys, new_values)
```

```python
import functools
import math

import jax
import jax.numpy as jnp
from jax import lax
from jax.experimental import pallas as pl
from jax.experimental.pallas import tpu as pltpu
from jax.sharding import PartitionSpec as P

HD = 128
EPG = 4
LANES = 128
MESH = pl.DeviceIdType.MESH
BF = jnp.bfloat16
F32 = jnp.float32

norm_eps = 1e-06


def dot(a, b):
    return jnp.dot(a, b, preferred_element_type=F32)


def silu(v):
    return v / (1.0 + jnp.exp(-v))


def sigmoid(v):
    return 1.0 / (1.0 + jnp.exp(-v))


def layer_kernel(
    n_ep,
    n_tp,
    tok_ref, gain_a_ref, mix_ref, gain_f_ref, len_ref, shift_ref, ids_ref, rw_ref,
    wq_h, wk_h, wv_h, kc_h, vc_h, wo_h, wdg_h, wdu_h, weg_h, weu_h, wed_h, wdd_h,
    mixed_ref, nk_ref, nv_ref,
    wqkv, kc, vc, wo, wdg, wdu, weg, weu, wed, wdd,
    qkv_s, qkv_r, mix_all, att_all, out_s, out_r, mid_own, mid_all, x_own, x_all,
    den_s, den_r, hid_own, hid_all, exp_s, exp_r, fin_s, fin_r, row_own, row_all,
    tok_f, score, att, part, xs, acc_g, acc_u, hid, total,
    w_sem, ep_ss, ep_rs, tp_ss, tp_rs,
):
    ep, tp = lax.axis_index("ep"), lax.axis_index("tp")
    batch, cols = tok_ref.shape
    seqs = batch // n_ep
    rows = batch // n_tp
    width = wq_h.shape[1]
    heads = width // HD
    length = kc.shape[1]
    ff = wdg.shape[1]
    local_experts = weg.shape[0]
    d_model = weg.shape[1]

    loads = {}

    def load(name, src, dst, k):
        loads[name] = pltpu.make_async_copy(src, dst, w_sem.at[k])
        loads[name].start()

    load("q", wq_h, wqkv.at[:, pl.ds(0, width)], 0)
    load("k", wk_h, wqkv.at[:, pl.ds(width, width)], 1)
    load("v", wv_h, wqkv.at[:, pl.ds(2 * width, width)], 2)
    load("kc", kc_h, kc, 3)
    load("vc", vc_h, vc, 4)
    load("wo", wo_h, wo, 5)
    load("wdg", wdg_h, wdg, 6)
    load("wdu", wdu_h, wdu, 7)
    load("weg", weg_h, weg, 8)
    load("weu", weu_h, weu, 9)
    load("wed", wed_h, wed, 10)
    load("wdd", wdd_h, wdd, 11)

    barrier = pltpu.get_barrier_semaphore()
    for d in range(1, n_ep):
        pl.semaphore_signal(
            barrier, inc=1, device_id={"ep": lax.rem(ep + d, n_ep)}, device_id_type=MESH
        )
    for d in range(1, n_tp):
        pl.semaphore_signal(
            barrier, inc=1, device_id={"tp": lax.rem(tp + d, n_tp)}, device_id_type=MESH
        )

    def send(axis, stage, src, dst):
        me, n, ss, rs = (ep, n_ep, ep_ss, ep_rs) if axis == "ep" else (tp, n_tp, tp_ss, tp_rs)
        copies = []
        for d in range(1, n):
            peer = lax.rem(me + d, n)
            copy = pltpu.make_async_remote_copy(
                src_ref=src(peer, d),
                dst_ref=dst(me, d),
                send_sem=ss.at[stage, d],
                recv_sem=rs.at[stage, d],
                device_id={axis: peer},
                device_id_type=MESH,
            )
            copy.start()
            copies.append(copy)
        return copies

    def finish(copies):
        for copy in copies:
            copy.wait()

    tokens = tok_ref[...].astype(F32)
    tok_f[...] = tokens
    scaled_in = (tokens * gain_a_ref[...].astype(F32)).astype(BF)
    for name in ("q", "k", "v"):
        loads[name].wait()
    qkv_s[:, : 3 * width] = dot(scaled_in, wqkv[...])
    qkv_s[:, 3 * width :] = jnp.broadcast_to(
        jnp.sum(tokens * tokens, axis=1, keepdims=True), (batch, LANES)
    )
    pl.semaphore_wait(barrier, n_ep + n_tp - 2)
    copies = send(
        "ep", 0, lambda peer, d: qkv_s.at[pl.ds(peer * seqs, seqs)], lambda me, d: qkv_r.at[d]
    )
    mix_copies = send("ep", 1, lambda peer, d: mix_ref, lambda me, d: mix_all.at[d])
    joint = qkv_s[pl.ds(ep * seqs, seqs), :]
    finish(copies)
    for d in range(1, n_ep):
        joint = joint + qkv_r[d]
    inv_first = lax.rsqrt(joint[:, 3 * width : 3 * width + 1] / d_model + norm_eps)
    joint = joint[:, : 3 * width] * inv_first
    queries = joint[:, :width].astype(BF).astype(F32)
    nk_ref[...] = joint[:, width : 2 * width].astype(BF)
    nv_ref[...] = joint[:, 2 * width :].astype(BF)

    lane_head = lax.broadcasted_iota(jnp.int32, (seqs, width), 1) // HD
    head_query = jnp.concatenate(
        [jnp.where(lane_head == h, queries, 0.0) for h in range(heads)], axis=0
    ).astype(BF)
    loads["kc"].wait()
    for s in range(seqs):
        found = lax.dot_general(
            head_query, kc[s], (((1,), (1,)), ((), ())), preferred_element_type=F32
        )
        for h in range(heads):
            score[h * seqs + s : h * seqs + s + 1, :] = found[h * seqs + s : h * seqs + s + 1, :]
    all_rows = heads * seqs
    scores = score[...] * (1.0 / math.sqrt(HD)) + shift_ref[...]
    live = lax.broadcasted_iota(jnp.int32, (all_rows, length), 1) < len_ref[...]
    tail = jnp.log1p(jnp.exp(-jnp.abs(scores)))
    soft = jnp.where(live, jnp.maximum(scores, 0.0) + tail, 0.0)
    chunks = length // LANES
    stacked = jnp.concatenate(
        [soft[:, c * LANES : (c + 1) * LANES] for c in range(chunks)], axis=0
    )
    later = (
        lax.broadcasted_iota(jnp.int32, (LANES, LANES), 0)
        > lax.broadcasted_iota(jnp.int32, (LANES, LANES), 1)
    ).astype(F32).astype(BF)
    high = stacked.astype(BF)
    rest = stacked - high.astype(F32)
    mid = rest.astype(BF)
    low = (rest - mid.astype(F32)).astype(BF)
    inner = dot(high, later) + (dot(mid, later) + dot(low, later))
    sums = jnp.sum(stacked, axis=1, keepdims=True)
    running = jnp.zeros((all_rows, 1), F32)
    pieces = [None] * chunks
    for c in reversed(range(chunks)):
        pieces[c] = inner[c * all_rows : (c + 1) * all_rows] + running
        running = running + sums[c * all_rows : (c + 1) * all_rows]
    later_sum = jnp.concatenate(pieces, axis=1)
    stick = jnp.where(
        live, jnp.exp(jnp.minimum(scores, 0.0) - tail - later_sum), 0.0
    ).astype(BF)
    loads["vc"].wait()
    for s in range(seqs):
        found = dot(stick, vc[s])
        for h in range(heads):
            att[s : s + 1, h * HD : (h + 1) * HD] = found[
                h * seqs + s : h * seqs + s + 1, h * HD : (h + 1) * HD
            ]
    att_all[ep] = att[...].astype(BF)
    copies = send("ep", 2, lambda peer, d: att_all.at[ep], lambda me, d: att_all.at[me])
    finish(mix_copies)
    loads["wo"].wait()
    finish(copies)

    part[...] = dot(att_all[...].reshape(batch, width), wo[...])
    for t in range(n_tp):
        out_s[t] = part[t * rows : (t + 1) * rows, :].astype(BF)
    copies = send("tp", 0, lambda peer, d: out_s.at[peer], lambda me, d: out_r.at[d])
    my_rows = pl.ds(pl.multiple_of(tp * rows, rows), rows)
    attn_out = part[my_rows, :]
    finish(copies)
    for d in range(1, n_tp):
        attn_out = attn_out + out_r[d].astype(F32)
    mid_own[...] = (tok_f[my_rows, :] + attn_out).astype(BF)
    mid_all[tp] = mid_own[...]
    copies = send("tp", 1, lambda peer, d: mid_own, lambda me, d: mid_all.at[me])
    finish(copies)
    middle = jnp.concatenate([mid_all[t].astype(F32) for t in range(n_tp)], axis=0)
    x_own[...] = middle.astype(BF)
    x_copies = send("ep", 3, lambda peer, d: x_own, lambda me, d: x_all.at[d])

    def features(d, block, squares, mixing):
        owner = lax.rem(ep - d + n_ep, n_ep)
        at = pl.ds(pl.multiple_of(owner * cols, cols), cols)
        scaled = (block * gain_f_ref[:, at].astype(F32)).astype(BF)
        xs[d] = scaled
        mix_row = mix_ref[0:1, :] if d == 0 else mix_all[d, 0:1, :]
        squares = squares + jnp.sum(block * block, axis=1, keepdims=True)
        mixing = mixing + jnp.sum(scaled.astype(F32) * mix_row, axis=1, keepdims=True)
        return at, squares, mixing

    def experts(d, at):
        def one(e, carry):
            gate = dot(xs[d], weg[e, at, :])
            up = dot(xs[d], weu[e, at, :])
            if d == 0:
                acc_g[e] = gate
                acc_u[e] = up
            else:
                acc_g[e] = acc_g[e] + gate
                acc_u[e] = acc_u[e] + up
            return carry

        lax.fori_loop(0, local_experts, one, 0)

    zero = jnp.zeros((batch, 1), F32)
    at, squares, mixing = features(0, middle, zero, zero)
    loads["wdg"].wait()
    loads["wdu"].wait()
    part[:, :ff] = dot(xs[0], wdg[...])
    total[:, :ff] = dot(xs[0], wdu[...])
    for e in range(n_ep):
        den_s[e, :, :ff] = part[e * seqs : (e + 1) * seqs, :ff].astype(BF)
        den_s[e, :, ff:] = total[e * seqs : (e + 1) * seqs, :ff].astype(BF)
    den_copies = send("ep", 4, lambda peer, d: den_s.at[peer], lambda me, d: den_r.at[d])
    my_seqs = pl.ds(pl.multiple_of(ep * seqs, seqs), seqs)
    dense_pre = part[my_seqs, :ff]
    dense_lin = total[my_seqs, :ff]
    loads["weg"].wait()
    loads["weu"].wait()
    experts(0, at)
    for d in range(1, n_ep):
        x_copies[d - 1].wait()
        at, squares, mixing = features(d, x_all[d].astype(F32), squares, mixing)
        experts(d, at)
    inv_second = lax.rsqrt(squares / d_model + norm_eps)
    mix_gate = sigmoid(mixing * inv_second)

    total[:, :LANES] = jnp.broadcast_to(inv_second, (batch, LANES))
    my_inv = total[my_seqs, :LANES][:, :1]
    finish(den_copies)
    for d in range(1, n_ep):
        dense_pre = dense_pre + den_r[d, :, :ff].astype(F32)
        dense_lin = dense_lin + den_r[d, :, ff:].astype(F32)
    hid_own[...] = (silu(dense_pre * my_inv) * (dense_lin * my_inv)).astype(BF)
    hid_all[ep] = hid_own[...]
    hid_copies = send("ep", 5, lambda peer, d: hid_own, lambda me, d: hid_all.at[me])

    for e in range(local_experts):
        hid[e] = (silu(acc_g[e] * inv_second) * (acc_u[e] * inv_second)).astype(BF)

    loads["wed"].wait()

    def down(owner):
        at = pl.ds(pl.multiple_of(owner * cols, cols), cols)
        total[...] = jnp.zeros_like(total)

        def one(e, carry):
            mine = ids_ref[...] == ep * local_experts + e
            weight = jnp.sum(jnp.where(mine, rw_ref[...], 0.0), axis=1, keepdims=True)
            total[...] += dot(hid[e], wed[e, :, at]) * weight
            return carry

        lax.fori_loop(0, local_experts, one, 0)

    exp_copies = []
    for d in range(1, n_ep):
        peer = lax.rem(ep + d, n_ep)
        down(peer)
        exp_s[d] = total[...].astype(BF)
        copy = pltpu.make_async_remote_copy(
            src_ref=exp_s.at[d],
            dst_ref=exp_r.at[d],
            send_sem=ep_ss.at[6, d],
            recv_sem=ep_rs.at[6, d],
            device_id={"ep": peer},
            device_id_type=MESH,
        )
        copy.start()
        exp_copies.append(copy)
    down(ep)
    loads["wdd"].wait()
    finish(hid_copies)
    total[...] += dot(hid_all[...].reshape(batch, ff), wdd[...]) * mix_gate
    for d in range(1, n_ep):
        exp_copies[d - 1].wait()
        total[...] += exp_r[d].astype(F32)

    for t in range(n_tp):
        fin_s[t] = total[t * rows : (t + 1) * rows, :].astype(BF)
    copies = send("tp", 2, lambda peer, d: fin_s.at[peer], lambda me, d: fin_r.at[d])
    result = total[my_rows, :] + mid_own[...].astype(F32)
    finish(copies)
    for d in range(1, n_tp):
        result = result + fin_r[d].astype(F32)
    row_own[...] = result.astype(BF)
    row_all[tp] = row_own[...]
    copies = send("tp", 3, lambda peer, d: row_own, lambda me, d: row_all.at[me])
    finish(copies)
    mixed_ref[...] = jnp.concatenate(
        [row_all[t].astype(F32) for t in range(n_tp)], axis=0
    ).astype(BF)


def on_device(
    n_ep,
    n_tp,
    tokens,
    gain_attn,
    w_query,
    w_key,
    w_value,
    w_output,
    key_cache,
    value_cache,
    lengths,
    score_shift,
    gain_ffn,
    w_mix,
    w_dense_gate,
    w_dense_up,
    w_dense_down,
    route_group,
    route_inner,
    route_weight,
    w_exp_gate,
    w_exp_up,
    w_exp_down,
):
    batch, cols = tokens.shape
    seqs, rows = batch // n_ep, batch // n_tp
    width = w_query.shape[1]
    heads = width // HD
    length = key_cache.shape[1]
    ff = w_dense_gate.shape[1]
    local_experts, d_model, unit = w_exp_gate.shape
    vm, hbm = pl.BlockSpec(memory_space=pltpu.VMEM), pl.BlockSpec(memory_space=pl.ANY)
    small = (
        tokens,
        gain_attn.reshape(1, cols),
        jnp.broadcast_to(w_mix.astype(F32)[None, :], (8, cols)),
        gain_ffn.reshape(1, d_model),
        jnp.tile(lengths, heads)[:, None],
        jnp.repeat(score_shift, seqs)[:, None],
        route_group[:, None] * EPG + route_inner,
        route_weight,
    )
    large = (
        w_query, w_key, w_value, key_cache, value_cache, w_output,
        w_dense_gate, w_dense_up, w_exp_gate, w_exp_up, w_exp_down, w_dense_down,
    )

    def buf(*shape, kind=BF):
        return pltpu.VMEM(shape, kind)

    scratch = [
        buf(cols, 3 * width),
        buf(*key_cache.shape),
        buf(*value_cache.shape),
        buf(*w_output.shape),
        buf(*w_dense_gate.shape),
        buf(*w_dense_up.shape),
        buf(*w_exp_gate.shape),
        buf(*w_exp_up.shape),
        buf(*w_exp_down.shape),
        buf(*w_dense_down.shape),
        buf(batch, 3 * width + LANES, kind=F32),
        buf(n_ep, seqs, 3 * width + LANES, kind=F32),
        buf(n_ep, 8, cols, kind=F32),
        buf(n_ep, seqs, width),
        buf(n_tp, rows, cols),
        buf(n_tp, rows, cols),
        buf(rows, cols),
        buf(n_tp, rows, cols),
        buf(batch, cols),
        buf(n_ep, batch, cols),
        buf(n_ep, seqs, 2 * ff),
        buf(n_ep, seqs, 2 * ff),
        buf(seqs, ff),
        buf(n_ep, seqs, ff),
        buf(n_ep, batch, cols),
        buf(n_ep, batch, cols),
        buf(n_tp, rows, cols),
        buf(n_tp, rows, cols),
        buf(rows, cols),
        buf(n_tp, rows, cols),
        buf(batch, cols, kind=F32),
        buf(heads * seqs, length, kind=F32),
        buf(seqs, width, kind=F32),
        buf(batch, cols, kind=F32),
        buf(n_ep, batch, cols),
        buf(local_experts, batch, unit, kind=F32),
        buf(local_experts, batch, unit, kind=F32),
        buf(local_experts, batch, unit),
        buf(batch, cols, kind=F32),
        pltpu.SemaphoreType.DMA((12,)),
        pltpu.SemaphoreType.DMA((7, n_ep)),
        pltpu.SemaphoreType.DMA((7, n_ep)),
        pltpu.SemaphoreType.DMA((4, n_tp)),
        pltpu.SemaphoreType.DMA((4, n_tp)),
    ]
    return pl.pallas_call(
        functools.partial(layer_kernel, n_ep, n_tp),
        out_shape=(
            jax.ShapeDtypeStruct((batch, cols), BF),
            jax.ShapeDtypeStruct((seqs, width), BF),
            jax.ShapeDtypeStruct((seqs, width), BF),
        ),
        in_specs=[vm] * len(small) + [hbm] * len(large),
        out_specs=(vm, vm, vm),
        scratch_shapes=scratch,
        compiler_params=pltpu.CompilerParams(
            collective_id=0, has_side_effects=True, vmem_limit_bytes=62 * 1024 * 1024
        ),
        name="layer",
    )(*small, *large)


def solution(mesh):
    placed = (
        P(None, "ep"),
        P("ep"),
        P("ep", "tp"),
        P("ep", "tp"),
        P("ep", "tp"),
        P("tp", "ep"),
        P("ep", None, "tp"),
        P("ep", None, "tp"),
        P("ep"),
        P("tp"),
        P(),
        P("ep"),
        P("ep", "tp"),
        P("ep", "tp"),
        P("tp", "ep"),
        P(),
        P(),
        P(),
        P("ep", None, "tp"),
        P("ep", None, "tp"),
        P("ep", "tp", None),
    )
    return jax.shard_map(
        functools.partial(on_device, mesh.shape["ep"], mesh.shape["tp"]),
        mesh=mesh,
        in_specs=placed,
        out_specs=(P(None, "ep"), P("ep", "tp"), P("ep", "tp")),
        check_vma=False,
    )
```
